32 devices in a mesh: grp: 2 (over x), kv: 4 (over z), tp: 4 (over y, core).
Axes of the slice: x: 2, y: 2, z: 4, core: 2. Of those that a mesh axis runs over, the one named last changes fastest.
Arguments:
- tokens: bfloat16 [16, 4096], P('grp', 'tp'), parts along dimension 0, may hold values from -50 to 50
- pre_gain: float32 [4096], P('tp'), may hold values from 0.1 to 1.9
- gate_first: bfloat16 [4096, 11264], P('tp', 'kv'), may hold values from -0.09375 to 0.09375
- up_first: bfloat16 [4096, 11264], P('tp', 'kv'), may hold values from -0.09375 to 0.09375
- down_first: bfloat16 [11264, 4096], P('kv', 'tp'), may hold values from -0.0546875 to 0.0546875
- mix_gain: float32 [4096], P('tp'), may hold values from 0.1 to 1.9
- query_w: bfloat16 [4096, 4096], P('tp', 'kv'), may hold values from -0.09375 to 0.09375
- key_w: bfloat16 [4096, 4096], P('tp', 'kv'), may hold values from -0.09375 to 0.09375
- value_w: bfloat16 [4096, 4096], P('tp', 'kv'), may hold values from -0.09375 to 0.09375
- forget_w: bfloat16 [4096, 32], P('tp'), may hold values from -0.09375 to 0.09375
- key_cache: bfloat16 [16, 1024, 4096], P('grp', 'tp', 'kv'), parts along dimension 0, may hold values from -800 to 800
- value_cache: bfloat16 [16, 1024, 4096], P('grp', 'tp', 'kv'), parts along dimension 0, may hold values from -6 to 6
- gate_cache: float32 [16, 32, 1024], P('grp', 'kv', 'tp'), parts along dimension 0, may hold values from -130 to 0, as said below
- lengths: int32 [16], P('grp'), parts along dimension 0, may hold values from 64 to 1024, as said below
- out_w: bfloat16 [4096, 4096], P('kv', 'tp'), may hold values from -0.09375 to 0.09375
- post_gain: float32 [4096], P('tp'), may hold values from 0.1 to 1.9
- gate_second: bfloat16 [4096, 11264], P('tp', 'kv'), may hold values from -0.09375 to 0.09375
- up_second: bfloat16 [4096, 11264], P('tp', 'kv'), may hold values from -0.09375 to 0.09375
- down_second: bfloat16 [11264, 4096], P('kv', 'tp'), may hold values from -0.0546875 to 0.0546875
Outputs:
- out: bfloat16 [16, 4096], P('grp', 'tp'), parts along dimension 0
The draws below stay inside these ranges and needn't reach their ends.
There are 2 independent parts, one for each index of `grp`. The reference program is written for one: setup_inputs(seed, part) draws one part's arguments, and reference() takes and returns one part's arrays. A program takes and returns all parts, laid end to end along the dimension named above; an argument that names none is the same for every part. Nothing has to cross between parts.
Inputs may be any that keep to these rules, and one draw needn't show every extreme that they name: `lengths`: each sequence's count of live cache positions; one sequence has all 1024 in every draw. `gate_cache`: at a live position p of sequence b, the sum of the log forget values of positions p + 1 to lengths[b] - 1 (zero at the last live position); never positive; zero beyond the live positions.
All inputs are finite; a program needn't handle non-finite values.
Results may differ from the reference program's by a relative error of at most 0.015.
Values may be sent and summed in bfloat16 or wider, within the bound.
A program may use at most 128 MiB of HBM per device.

```python
import math
import jax
import jax.numpy as jnp
from jax import lax

D = 4096
FF = 11264
ATTENTION_HEADS = 32
HEAD_DIM = 128
DECODE_SEQUENCES = 8
CTX_DEV = 256
CONTEXT_SLOTS = 1024


def draw_tokens(key, part):
    column = jnp.arange(D, dtype=jnp.float32) / D
    base = jnp.clip(jax.random.normal(jax.random.fold_in(key, 11), (DECODE_SEQUENCES, D), jnp.float32), -4.0, 4.0)
    rising = 0.5 * 4.0 ** column
    jitter = jnp.exp(jax.random.uniform(jax.random.fold_in(key, 13), (1, D), jnp.float32, -0.5, 0.5))
    row_scale = jnp.exp(jax.random.uniform(jax.random.fold_in(key, 14), (DECODE_SEQUENCES, 1), jnp.float32, math.log(0.5), math.log(2.0)))
    return (base * rising[None, :] * jitter * row_scale).astype(jnp.bfloat16)


def live_lengths(key):
    random_subkey = jax.random.fold_in(key, 21)
    spread = jax.random.randint(jax.random.fold_in(random_subkey, 1), (DECODE_SEQUENCES,), CONTEXT_SLOTS // 16, CONTEXT_SLOTS // 3 + 1)
    longest = jax.random.randint(jax.random.fold_in(random_subkey, 2), (), 0, DECODE_SEQUENCES)
    return jnp.where(jnp.arange(DECODE_SEQUENCES, dtype=jnp.int32) == longest, CONTEXT_SLOTS, spread).astype(jnp.int32)


def draw_lengths(key, part):
    return live_lengths(key)


def draw_gate_cache(key, part):
    lengths = live_lengths(key)
    random_subkey = jax.random.fold_in(key, 31)
    ranks = jax.random.permutation(jax.random.fold_in(random_subkey, 1), ATTENTION_HEADS)
    fast_count = ATTENTION_HEADS // 2
    is_fast = ranks < fast_count
    decay_speed = jnp.where(is_fast, 1.0 / 40.0, 0.5 / CONTEXT_SLOTS).astype(jnp.float32)
    blocks = CONTEXT_SLOTS // CTX_DEV
    block_multiplier = jnp.exp(jax.random.uniform(jax.random.fold_in(random_subkey, 2), (DECODE_SEQUENCES, ATTENTION_HEADS, blocks), jnp.float32, -0.7, 0.7))
    block_multiplier = jnp.repeat(block_multiplier, CTX_DEV, axis=2)
    coarse_estimate = jax.random.uniform(jax.random.fold_in(random_subkey, 3), (DECODE_SEQUENCES, ATTENTION_HEADS, CONTEXT_SLOTS), jnp.float32, 0.5, 1.5)
    spike_position = jax.random.randint(jax.random.fold_in(random_subkey, 4), (DECODE_SEQUENCES, ATTENTION_HEADS, 2), 0, CONTEXT_SLOTS)
    spike_extent = jnp.log(jax.random.uniform(jax.random.fold_in(random_subkey, 5), (DECODE_SEQUENCES, ATTENTION_HEADS, 2, 1), jnp.float32, 0.5, 0.8))
    slot_positions = jnp.arange(CONTEXT_SLOTS, dtype=jnp.int32)
    spike_events = jnp.sum(jnp.where(slot_positions[None, None, None, :] == spike_position[:, :, :, None], spike_extent, 0.0), axis=2)
    gate_logarithm = -decay_speed[None, :, None] * block_multiplier * coarse_estimate + spike_events
    running = jnp.cumsum(gate_logarithm, axis=2)
    last_index = jnp.broadcast_to((lengths - 1)[:, None, None], (DECODE_SEQUENCES, ATTENTION_HEADS, 1))
    newest = jnp.take_along_axis(running, last_index, axis=2)
    live = slot_positions[None, None, :] < lengths[:, None, None]
    return jnp.where(live, newest - running, 0.0).astype(jnp.float32)


def draw_key_cache(key, part):
    base = jnp.clip(jax.random.normal(jax.random.fold_in(key, 41), (DECODE_SEQUENCES, CONTEXT_SLOTS, ATTENTION_HEADS * HEAD_DIM), jnp.float32), -6.0, 6.0)
    return base.astype(jnp.bfloat16)


def level_of(own_key, shape, cuts, low, largest):
    loudness, own = 1.0, jax.random.fold_in(own_key, 6)
    for position, shards_of in cuts:
        steps = jnp.exp(jax.random.uniform(jax.random.fold_in(own, position), (shards_of,), jnp.float32, low / len(cuts), largest / len(cuts)))
        loudness = loudness * jnp.repeat(steps, shape[position] // shards_of).reshape([-1 if axis == position else 1 for axis in range(len(shape))])
    return loudness


def normal_values(rng, shape, deviation, reach, split=(), kind=jnp.bfloat16):
    values = deviation * jax.random.normal(rng, shape, jnp.float32)
    if split:
        values = values * level_of(rng, shape, split, -0.22, 0.18)
    return jnp.clip(values, -reach, reach).astype(kind)


def setup_inputs(seed: int = 0, part: int = 0) -> dict:
    keys = jax.random.split(jax.random.key(seed), 20)
    part_splits = jax.random.split(jax.random.fold_in(keys[19], part), 20)
    return {
        "tokens": draw_tokens(jax.random.fold_in(jax.random.fold_in(keys[19], part), 71), part),
        "pre_gain": jnp.clip(1.0 + 0.18 * jax.random.normal(keys[1], (D,), jnp.float32), 0.1, 1.9),
        "gate_first": normal_values(keys[2], (D, FF), D ** -0.5, 0.09375, ((0, 4), (1, 4))),
        "up_first": normal_values(keys[3], (D, FF), D ** -0.5, 0.09375, ((0, 4), (1, 4))),
        "down_first": normal_values(keys[4], (FF, D), FF ** -0.5, 0.0546875, ((0, 4), (1, 4))),
        "mix_gain": jnp.clip(1.0 + 0.18 * jax.random.normal(keys[5], (D,), jnp.float32), 0.1, 1.9),
        "query_w": normal_values(keys[6], (D, ATTENTION_HEADS * HEAD_DIM), D ** -0.5, 0.09375, ((0, 4), (1, 4))),
        "key_w": normal_values(keys[7], (D, ATTENTION_HEADS * HEAD_DIM), D ** -0.5, 0.09375, ((0, 4), (1, 4))),
        "value_w": normal_values(keys[8], (D, ATTENTION_HEADS * HEAD_DIM), D ** -0.5, 0.09375, ((0, 4), (1, 4))),
        "forget_w": normal_values(keys[9], (D, ATTENTION_HEADS), D ** -0.5, 0.09375, ((0, 4),)),
        "key_cache": draw_key_cache(jax.random.fold_in(jax.random.fold_in(keys[19], part), 71), part),
        "value_cache": normal_values(part_splits[11], (DECODE_SEQUENCES, CONTEXT_SLOTS, ATTENTION_HEADS * HEAD_DIM), 1.0, 6.0, ((1, 4), (2, 4))),
        "gate_cache": draw_gate_cache(jax.random.fold_in(jax.random.fold_in(keys[19], part), 71), part),
        "lengths": draw_lengths(jax.random.fold_in(jax.random.fold_in(keys[19], part), 71), part),
        "out_w": normal_values(keys[14], (ATTENTION_HEADS * HEAD_DIM, D), (ATTENTION_HEADS * HEAD_DIM) ** -0.5, 0.09375, ((0, 4), (1, 4))),
        "post_gain": jnp.clip(1.0 + 0.18 * jax.random.normal(keys[15], (D,), jnp.float32), 0.1, 1.9),
        "gate_second": normal_values(keys[16], (D, FF), D ** -0.5, 0.09375, ((0, 4), (1, 4))),
        "up_second": normal_values(keys[17], (D, FF), D ** -0.5, 0.09375, ((0, 4), (1, 4))),
        "down_second": normal_values(keys[18], (FF, D), FF ** -0.5, 0.0546875, ((0, 4), (1, 4))),
    }


EPSILON = 1e-06
MASKED = -1e+30

def half_step(tok_rows, gain_part, w_gate, w_up, w_down):
    widened = tok_rows.astype(jnp.float32)
    sq_total = lax.optimization_barrier(jnp.sum(widened * widened, axis=1, keepdims=True))
    norm_scale = lax.rsqrt(sq_total / D + EPSILON)
    weighted = (widened * gain_part).astype(jnp.bfloat16)
    gate_sum = norm_scale * jnp.dot(weighted, w_gate, preferred_element_type=jnp.float32)
    up_sum = norm_scale * jnp.dot(weighted, w_up, preferred_element_type=jnp.float32)
    hidden = (jax.nn.silu(gate_sum) * up_sum).astype(jnp.bfloat16)
    down_sum = jnp.dot(hidden, w_down, preferred_element_type=jnp.float32)
    return (widened + 0.5 * down_sum).astype(jnp.bfloat16)

def attend(after_first, mix_gain, query_w, key_w, value_w, forget_w, key_cache, value_cache, gate_cache, lengths):
    widened = after_first.astype(jnp.float32)
    sq_total = lax.optimization_barrier(jnp.sum(widened * widened, axis=1, keepdims=True))
    norm_scale = lax.rsqrt(sq_total / D + EPSILON)
    weighted = (widened * mix_gain).astype(jnp.bfloat16)
    query = (norm_scale * jnp.dot(weighted, query_w, preferred_element_type=jnp.float32)).astype(jnp.bfloat16)
    key_new = (norm_scale * jnp.dot(weighted, key_w, preferred_element_type=jnp.float32)).astype(jnp.bfloat16)
    value_new = (norm_scale * jnp.dot(weighted, value_w, preferred_element_type=jnp.float32)).astype(jnp.bfloat16)
    log_forget = jax.nn.log_sigmoid(norm_scale * jnp.dot(weighted, forget_w, preferred_element_type=jnp.float32))
    query_heads = query.reshape(DECODE_SEQUENCES, ATTENTION_HEADS, HEAD_DIM).astype(jnp.float32)

    def one_block(index):
        offset = index * CTX_DEV
        key_block = lax.dynamic_slice_in_dim(key_cache, offset, CTX_DEV, 1).reshape(DECODE_SEQUENCES, CTX_DEV, ATTENTION_HEADS, HEAD_DIM).astype(jnp.float32)
        value_block = lax.dynamic_slice_in_dim(value_cache, offset, CTX_DEV, 1).reshape(DECODE_SEQUENCES, CTX_DEV, ATTENTION_HEADS, HEAD_DIM).astype(jnp.float32)
        gate_block = lax.dynamic_slice_in_dim(gate_cache, offset, CTX_DEV, 2)
        scores = jnp.einsum('bhd,bphd->bhp', query_heads, key_block) * HEAD_DIM ** (-0.5)
        scores = scores + gate_block + log_forget[:, :, None]
        slot_positions = offset + jnp.arange(CTX_DEV, dtype=jnp.int32)
        is_live = slot_positions[None, None, :] < lengths[:, None, None]
        local_top = lax.optimization_barrier(jnp.max(jnp.where(is_live, scores, MASKED), axis=2))
        local_probs = jnp.where(is_live, jnp.exp(scores - local_top[:, :, None]), 0.0)
        local_mass = lax.optimization_barrier(jnp.sum(local_probs, axis=2))
        rounded = local_probs.astype(jnp.bfloat16).astype(jnp.float32)
        local_sum = jnp.einsum('bhp,bphd->bhd', rounded, value_block).astype(jnp.bfloat16)
        return (local_top, local_mass, local_sum)
    piece_top, masses, piece_sum = lax.map(one_block, jnp.arange(CONTEXT_SLOTS // CTX_DEV, dtype=jnp.int32))
    overall = lax.optimization_barrier(jnp.max(piece_top, axis=0))
    factors = jnp.exp(piece_top - overall[None])
    run_mass = lax.optimization_barrier(jnp.sum(masses * factors, axis=0))
    run_sum = lax.optimization_barrier(jnp.sum(piece_sum.astype(jnp.float32) * factors[:, :, :, None], axis=0))
    new_heads = key_new.reshape(DECODE_SEQUENCES, ATTENTION_HEADS, HEAD_DIM).astype(jnp.float32)
    own_score = lax.optimization_barrier(jnp.sum(query_heads * new_heads, axis=2)) * HEAD_DIM ** (-0.5)
    highest = jnp.maximum(overall, own_score)
    rescale = jnp.exp(overall - highest)
    own_weight = jnp.exp(own_score - highest)
    own_values = value_new.reshape(DECODE_SEQUENCES, ATTENTION_HEADS, HEAD_DIM).astype(jnp.float32)
    numer = run_sum * rescale[:, :, None] + own_weight[:, :, None] * own_values
    denom = run_mass * rescale + own_weight
    return (numer / denom[:, :, None]).astype(jnp.bfloat16).reshape(DECODE_SEQUENCES, ATTENTION_HEADS * HEAD_DIM)

def reference(tokens, pre_gain, gate_first, up_first, down_first, mix_gain, query_w, key_w, value_w, forget_w, key_cache, value_cache, gate_cache, lengths, out_w, post_gain, gate_second, up_second, down_second):
    after_first = half_step(tokens, pre_gain, gate_first, up_first, down_first)
    attended = attend(after_first, mix_gain, query_w, key_w, value_w, forget_w, key_cache, value_cache, gate_cache, lengths)
    projected = jnp.dot(attended, out_w, preferred_element_type=jnp.float32)
    residual_two = (after_first.astype(jnp.float32) + projected).astype(jnp.bfloat16)
    return half_step(residual_two, post_gain, gate_second, up_second, down_second)
```

```python
import functools

import jax
import jax.numpy as jnp
from jax import lax
from jax.experimental import pallas as pl
from jax.experimental.pallas import tpu as pltpu
from jax.sharding import PartitionSpec as P

HEAD_DIM = 128
EPSILON = 1e-06
MASKED = -1e30
LANES = 128
MESH = pl.DeviceIdType.MESH
F32 = jnp.float32
BF16 = jnp.bfloat16


def chunk_width(columns, wanted=256):
    return wanted if columns % wanted == 0 else columns


def dot(a, b):
    return jnp.dot(a, b, preferred_element_type=F32)


class Exchange:
    def __init__(self, axis, count, buffer, send, recv, base):
        self.axis, self.count, self.buffer = axis, count, buffer
        self.send, self.recv, self.base = send, recv, base
        self.me = lax.axis_index(axis)

    def copy(self, step, window, out):
        me = self.me
        peer = lax.rem(me + step, self.count)
        origin = me if out else lax.rem(me + self.count - step, self.count)
        view = self.buffer.at[origin]
        if window is not None:
            view = view.at[:, pl.ds(*window)]
        slot = self.base + step - 1
        return pltpu.make_async_remote_copy(
            src_ref=view,
            dst_ref=view,
            send_sem=self.send.at[slot],
            recv_sem=self.recv.at[slot],
            device_id={self.axis: peer},
            device_id_type=MESH,
        )

    def start(self, window=None):
        for step in range(1, self.count):
            self.copy(step, window, True).start()

    def wait_recv(self, window=None):
        for step in range(1, self.count):
            self.copy(step, window, False).wait_recv()

    def wait_send(self, window=None):
        for step in range(1, self.count):
            self.copy(step, window, True).wait_send()


def body(n_tp, n_kv, dims, *refs):
    (
        tok_h, g1_h, wg1_h, wu1_h, wd1_h, g2_h, wq_h, wk_h, wv_h, wf_h, kc_h, vc_h, gc_h,
        len_s, wo_h, g3_h, wg2_h, wu2_h, wd2_h,
        out_ref,
        tok, g1, wg1, wu1, wd1, g2, wq, wk, wv, wf, kc, vc, gc, wo, g3, wg2, wu2, wd2,
        hid, osum, stats,
        x1a, x1b, xs1, xs2, xs3, xq, xkv, xo, xd1, xd2, xd3, xs4,
        local_sem, tp_send, tp_recv, kv_send, kv_recv,
    ) = refs
    batch, model, width, hidden, span, heads, d_full = dims
    me_tp = lax.axis_index("tp")
    me_kv = lax.axis_index("kv")

    barrier = pltpu.get_barrier_semaphore()
    for step in range(1, n_tp):
        pl.semaphore_signal(
            barrier, inc=1, device_id={"tp": lax.rem(me_tp + step, n_tp)}, device_id_type=MESH
        )
    for step in range(1, n_kv):
        pl.semaphore_signal(
            barrier, inc=1, device_id={"kv": lax.rem(me_kv + step, n_kv)}, device_id_type=MESH
        )

    used = [0]

    def load(source, target):
        copy = pltpu.make_async_copy(source, target, local_sem.at[used[0]])
        used[0] += 1
        copy.start()
        return copy

    def load_rows(source, target, pieces):
        rows = source.shape[0]
        if rows % pieces or (rows // pieces) % 16:
            pieces = 1
        size = rows // pieces
        return [
            load(source.at[pl.ds(i * size, size)], target.at[pl.ds(i * size, size)])
            for i in range(pieces)
        ]

    cw = chunk_width(hidden)
    n_chunks = hidden // cw

    def load_pair(wg_h, wu_h, wg, wu, c):
        cols = pl.ds(c * cw, cw)
        return [load(wg_h.at[:, cols], wg.at[:, cols]), load(wu_h.at[:, cols], wu.at[:, cols])]

    first_loads = [load(tok_h, tok), load(g1_h, g1)]
    pair1 = [load_pair(wg1_h, wu1_h, wg1, wu1, c) for c in range(n_chunks)]
    down1_loads = load_rows(wd1_h, wd1, 4)
    mix_loads = [load(g2_h, g2), load(wf_h, wf)]
    q_loads = load_rows(wq_h, wq, 2)
    k_loads = load_rows(wk_h, wk, 2)
    v_loads = load_rows(wv_h, wv, 2)
    key_loads = [load(gc_h, gc)] + load_rows(kc_h, kc, 1)
    val_loads = load_rows(vc_h, vc, 1)
    out_loads = load_rows(wo_h, wo, 2) + [load(g3_h, g3)]
    pair2 = [load_rows(wg2_h, wg2, 4) + load_rows(wu2_h, wu2, 4)] + [[]] * (n_chunks - 1)
    down2_loads = load_rows(wd2_h, wd2, 4)

    def wait_all(copies):
        for copy in copies:
            copy.wait()

    base_tp, base_kv = [0], [0]
    pending = []

    def tp_exchange(buffer):
        ex = Exchange("tp", n_tp, buffer, tp_send, tp_recv, base_tp[0])
        base_tp[0] += n_tp - 1
        return ex

    def kv_exchange(buffer):
        ex = Exchange("kv", n_kv, buffer, kv_send, kv_recv, base_kv[0])
        base_kv[0] += n_kv - 1
        return ex

    def begin(ex, window=None):
        ex.start(window)
        pending.append((ex, window))

    def total(buffer, count, rows=slice(None)):
        acc = buffer[0, rows].astype(F32)
        for j in range(1, count):
            acc = acc + buffer[j, rows].astype(F32)
        return acc

    lane = lax.broadcasted_iota(jnp.int32, (batch, LANES), 1)

    def half_step(rows, gain, pairs, wg, wu, down_loads, wd, x1, xs, xd, first):
        squares = jnp.sum(rows * rows, axis=1, keepdims=True)
        weighted = (rows * gain[...]).astype(BF16)
        xs[me_tp] = jnp.broadcast_to(squares, (batch, LANES))
        sq_ex = tp_exchange(xs)
        if first:
            pl.semaphore_wait(barrier, n_tp - 1 + n_kv - 1)
        begin(sq_ex)
        cut = (n_chunks + 1) // 2
        windows = []
        for lo, hi in ((0, cut), (cut, n_chunks)):
            if hi == lo:
                continue
            for c in range(lo, hi):
                wait_all(pairs[c])
                cols = pl.ds(c * cw, cw)
                both = jnp.concatenate([dot(weighted, wg[:, cols]), dot(weighted, wu[:, cols])], axis=0)
                x1[me_tp, :, cols] = both.astype(BF16)
            window = None if n_chunks == 1 else (lo * cw, (hi - lo) * cw)
            ex = tp_exchange(x1)
            begin(ex, window)
            windows.append((ex, window, slice(lo * cw, hi * cw)))
        sq_ex.wait_recv()
        scale = lax.rsqrt(total(xs, n_tp)[:, 0:1] / d_full + EPSILON)
        for ex, window, cols in windows:
            ex.wait_recv(window)
            acc = x1[0, :, cols].astype(F32)
            for j in range(1, n_tp):
                acc = acc + x1[j, :, cols].astype(F32)
            gate, up = scale * acc[:batch], scale * acc[batch:]
            hid[:, cols] = (gate / (1.0 + jnp.exp(-gate)) * up).astype(BF16)
        wait_all(down_loads)
        xd[me_kv] = dot(hid[...], wd[...]).astype(BF16)
        down_ex = kv_exchange(xd)
        begin(down_ex)
        down_ex.wait_recv()
        return (rows + 0.5 * total(xd, n_kv)).astype(BF16).astype(F32)

    wait_all(first_loads)
    after_first = half_step(
        tok[...].astype(F32), g1, pair1, wg1, wu1, down1_loads, wd1, x1a, xs1, xd1, True
    )

    squares = jnp.sum(after_first * after_first, axis=1, keepdims=True)
    wait_all(mix_loads)
    weighted = (after_first * g2[...]).astype(BF16)
    n_heads_all = wf.shape[1]
    forget = dot(weighted, wf[...])
    forget = jnp.concatenate([forget, jnp.zeros((batch, LANES - n_heads_all), F32)], axis=1)
    xs2[me_tp] = jnp.where(lane == LANES - 1, squares, forget)
    s_ex = tp_exchange(xs2)
    begin(s_ex)
    wait_all(q_loads)
    xq[me_tp] = dot(weighted, wq[...])
    q_ex = tp_exchange(xq)
    begin(q_ex)
    wait_all(k_loads)
    key_part = dot(weighted, wk[...])
    wait_all(v_loads)
    xkv[me_tp] = jnp.concatenate([key_part, dot(weighted, wv[...])], axis=0).astype(BF16)
    kv_ex = tp_exchange(xkv)
    begin(kv_ex)

    s_ex.wait_recv()
    small = total(xs2, n_tp)
    scale = lax.rsqrt(small[:, LANES - 1 :] / d_full + EPSILON)
    logits = scale * small
    log_all = jnp.minimum(logits, 0.0) - jnp.log(1.0 + jnp.exp(-jnp.abs(logits)))
    log_forget = log_all
    for k in range(1, n_kv):
        log_forget = jnp.where(
            me_kv == k, pltpu.roll(log_all, LANES - k * heads, 1), log_forget
        )
    q_ex.wait_recv()
    query = (scale * total(xq, n_tp)).astype(BF16).astype(F32)

    wait_all(key_loads)
    wait_all(val_loads)
    row_head = lax.broadcasted_iota(jnp.int32, (heads, width), 0)
    own_cols = row_head == lax.broadcasted_iota(jnp.int32, (heads, width), 1) // HEAD_DIM
    slots = me_tp * span + lax.broadcasted_iota(jnp.int32, (heads, span), 1)
    stat_row = lax.broadcasted_iota(jnp.int32, (heads, LANES), 0)
    stat_lane = lax.broadcasted_iota(jnp.int32, (heads, LANES), 1)
    half = LANES // 2
    for b in range(batch):
        spread = jnp.where(own_cols, query[b : b + 1, :], 0.0).astype(BF16)
        scores = lax.dot_general(
            spread, kc[b], (((1,), (1,)), ((), ())), preferred_element_type=F32
        ) * HEAD_DIM ** (-0.5)
        scores = scores + gc[b]
        live = slots < len_s[b]
        top = jnp.max(jnp.where(live, scores, MASKED), axis=1, keepdims=True)
        probs = jnp.where(live, jnp.exp(scores - top), 0.0)
        mass = jnp.sum(probs, axis=1, keepdims=True)
        mixed = dot(probs.astype(BF16), vc[b])
        osum[b : b + 1, :] = jnp.sum(jnp.where(own_cols, mixed, 0.0), axis=0, keepdims=True)
        placed = jnp.where(
            stat_row == stat_lane, top, jnp.where(stat_row + half == stat_lane, mass, 0.0)
        )
        stats[b : b + 1, :] = jnp.sum(placed, axis=0, keepdims=True)
    xs3[me_tp] = stats[...]
    st_ex = tp_exchange(xs3)
    begin(st_ex)
    xo[me_tp] = osum[...].astype(BF16)
    o_ex = tp_exchange(xo)
    begin(o_ex)

    kv_ex.wait_recv()
    kv_sum = total(xkv, n_tp)
    key_new = (scale * kv_sum[:batch]).astype(BF16).astype(F32)
    value_new = (scale * kv_sum[batch:]).astype(BF16).astype(F32)
    own = jnp.zeros((batch, LANES), F32)
    for h in range(heads):
        cols = slice(h * HEAD_DIM, (h + 1) * HEAD_DIM)
        own = jnp.where(
            lane == h, jnp.sum(query[:, cols] * key_new[:, cols], axis=1, keepdims=True), own
        )
    own = own * HEAD_DIM ** (-0.5)

    st_ex.wait_recv()
    tops = [xs3[j] + log_forget for j in range(n_tp)]
    highest = own
    for t in tops:
        highest = jnp.maximum(highest, t)
    factors = [jnp.exp(t - highest) for t in tops]
    own_factor = jnp.exp(own - highest)
    denom = own_factor
    for j in range(n_tp):
        denom = denom + factors[j] * pltpu.roll(xs3[j], half, 1)
    own_factor = own_factor / denom
    factors = [f / denom for f in factors]
    o_ex.wait_recv()
    pieces = []
    for h in range(heads):
        cols = slice(h * HEAD_DIM, (h + 1) * HEAD_DIM)
        acc = own_factor[:, h : h + 1] * value_new[:, cols]
        for j in range(n_tp):
            acc = acc + factors[j][:, h : h + 1] * xo[j, :, cols].astype(F32)
        pieces.append(acc.astype(BF16))
    attended = jnp.concatenate(pieces, axis=1)
    wait_all(out_loads)
    xd2[me_kv] = dot(attended, wo[...]).astype(BF16)
    p_ex = kv_exchange(xd2)
    begin(p_ex)
    p_ex.wait_recv()
    residual_two = (after_first + total(xd2, n_kv)).astype(BF16).astype(F32)

    result = half_step(
        residual_two, g3, pair2, wg2, wu2, down2_loads, wd2, x1b, xs4, xd3, False
    )
    out_ref[...] = result.astype(out_ref.dtype)
    for ex, window in pending:
        ex.wait_send(window)


def on_device(n_tp, n_kv, *args):
    (tokens, pre_gain, gate_first, up_first, down_first, mix_gain, query_w, key_w, value_w,
     forget_w, key_cache, value_cache, gate_cache, lengths, out_w, post_gain, gate_second,
     up_second, down_second) = args
    batch, model = tokens.shape
    hidden = gate_first.shape[1]
    width = query_w.shape[1]
    span = key_cache.shape[1]
    heads = width // HEAD_DIM
    d_full = model * n_tp
    row = lambda v: v.reshape(1, v.shape[0])
    operands = [tokens, row(pre_gain), gate_first, up_first, down_first, row(mix_gain), query_w,
                key_w, value_w, forget_w, key_cache, value_cache, gate_cache, lengths, out_w,
                row(post_gain), gate_second, up_second, down_second]
    lengths_at = 13
    any_spec = pl.BlockSpec(memory_space=pl.ANY)
    in_specs = [any_spec] * len(operands)
    in_specs[lengths_at] = pl.BlockSpec(memory_space=pltpu.SMEM)
    held = [pltpu.VMEM(a.shape, a.dtype) for i, a in enumerate(operands) if i != lengths_at]
    dims = (batch, model, width, hidden, span, heads, d_full)
    small = pltpu.VMEM((n_tp, batch, LANES), F32)
    cw = chunk_width(hidden)
    n_local = 2 * (hidden // cw) + 64
    tp_slots = 11 * (n_tp - 1)
    kv_slots = 3 * (n_kv - 1)
    scratch = held + [
        pltpu.VMEM((batch, hidden), BF16),
        pltpu.VMEM((batch, width), F32),
        pltpu.VMEM((batch, LANES), F32),
        pltpu.VMEM((n_tp, 2 * batch, hidden), BF16),
        pltpu.VMEM((n_tp, 2 * batch, hidden), BF16),
        small,
        small,
        small,
        pltpu.VMEM((n_tp, batch, width), F32),
        pltpu.VMEM((n_tp, 2 * batch, width), BF16),
        pltpu.VMEM((n_tp, batch, width), BF16),
        pltpu.VMEM((n_kv, batch, model), BF16),
        pltpu.VMEM((n_kv, batch, model), BF16),
        pltpu.VMEM((n_kv, batch, model), BF16),
        small,
        pltpu.SemaphoreType.DMA((n_local,)),
        pltpu.SemaphoreType.DMA((tp_slots,)),
        pltpu.SemaphoreType.DMA((tp_slots,)),
        pltpu.SemaphoreType.DMA((kv_slots,)),
        pltpu.SemaphoreType.DMA((kv_slots,)),
    ]
    return pl.pallas_call(
        functools.partial(body, n_tp, n_kv, dims),
        out_shape=jax.ShapeDtypeStruct(tokens.shape, tokens.dtype),
        in_specs=in_specs,
        out_specs=pl.BlockSpec(memory_space=pltpu.VMEM),
        scratch_shapes=scratch,
        compiler_params=pltpu.CompilerParams(
            collective_id=0, has_side_effects=True, vmem_limit_bytes=62 * 1024 * 1024
        ),
    )(*operands)


def solution(mesh):
    placed = (
        P("grp", "tp"),
        P("tp"),
        P("tp", "kv"),
        P("tp", "kv"),
        P("kv", "tp"),
        P("tp"),
        P("tp", "kv"),
        P("tp", "kv"),
        P("tp", "kv"),
        P("tp", None),
        P("grp", "tp", "kv"),
        P("grp", "tp", "kv"),
        P("grp", "kv", "tp"),
        P("grp"),
        P("kv", "tp"),
        P("tp"),
        P("tp", "kv"),
        P("tp", "kv"),
        P("kv", "tp"),
    )
    return jax.shard_map(
        functools.partial(on_device, mesh.shape["tp"], mesh.shape["kv"]),
        mesh=mesh,
        in_specs=placed,
        out_specs=P("grp", "tp"),
        check_vma=False,
    )
```

```python
import functools

import jax
import jax.numpy as jnp
from jax import lax
from jax.experimental import pallas as pl
from jax.experimental.pallas import tpu as pltpu
from jax.sharding import PartitionSpec as P

HEAD_DIM = 128
EPSILON = 1e-06
MASKED = -1e30
LANES = 128
WINDOWS = 4
KV_WINDOWS = 2
MESH = pl.DeviceIdType.MESH
F32 = jnp.float32
BF16 = jnp.bfloat16


def chunk_width(columns, wanted=256):
    return wanted if columns % wanted == 0 else columns


def dot(a, b):
    return jnp.dot(a, b, preferred_element_type=F32)


class Exchange:
    def __init__(self, axis, count, buffer, send, recv, base):
        self.axis, self.count, self.buffer = axis, count, buffer
        self.send, self.recv, self.base = send, recv, base
        self.me = lax.axis_index(axis)

    def copy(self, step, window, out):
        me = self.me
        peer = lax.rem(me + step, self.count)
        origin = me if out else lax.rem(me + self.count - step, self.count)
        view = self.buffer.at[origin]
        if window is not None:
            view = view.at[:, pl.ds(*window)]
        slot = self.base + step - 1
        return pltpu.make_async_remote_copy(
            src_ref=view,
            dst_ref=view,
            send_sem=self.send.at[slot],
            recv_sem=self.recv.at[slot],
            device_id={self.axis: peer},
            device_id_type=MESH,
        )

    def start(self, window=None):
        for step in range(1, self.count):
            self.copy(step, window, True).start()

    def wait_recv(self, window=None):
        for step in range(1, self.count):
            self.copy(step, window, False).wait_recv()

    def wait_send(self, window=None):
        for step in range(1, self.count):
            self.copy(step, window, True).wait_send()


def body(n_tp, n_kv, dims, *refs):
    (
        tok_h, g1_h, wg1_h, wu1_h, wd1_h, g2_h, wq_h, wk_h, wv_h, wf_h, kc_h, vc_h, gc_h,
        len_h, wo_h, g3_h, wg2_h, wu2_h, wd2_h,
        out_ref,
        tok, g1, wg1, wu1, wd1, g2, wq, wk, wv, wf, kc, vc, gc, wo, g3, wg2, wu2, wd2,
        hid, osum,
        x1a, x1b, xs1, xs2, xs3, xq, xkv, xo, xd1, xd2, xd3, xs4, lens,
        local_sem, tp_send, tp_recv, kv_send, kv_recv,
    ) = refs
    batch, model, width, hidden, span, heads, d_full = dims
    me_tp = lax.axis_index("tp")
    me_kv = lax.axis_index("kv")

    barrier = pltpu.get_barrier_semaphore()
    for step in range(1, n_tp):
        pl.semaphore_signal(
            barrier, inc=1, device_id={"tp": lax.rem(me_tp + step, n_tp)}, device_id_type=MESH
        )
    for step in range(1, n_kv):
        pl.semaphore_signal(
            barrier, inc=1, device_id={"kv": lax.rem(me_kv + step, n_kv)}, device_id_type=MESH
        )

    used = [0]

    def load(source, target):
        copy = pltpu.make_async_copy(source, target, local_sem.at[used[0]])
        used[0] += 1
        copy.start()
        return copy

    def load_rows(source, target, pieces):
        rows = source.shape[0]
        if rows % pieces or (rows // pieces) % 16:
            pieces = 1
        size = rows // pieces
        return [
            load(source.at[pl.ds(i * size, size)], target.at[pl.ds(i * size, size)])
            for i in range(pieces)
        ]

    cw = chunk_width(hidden)
    n_chunks = hidden // cw

    def load_pair(wg_h, wu_h, wg, wu, c):
        cols = pl.ds(c * cw, cw)
        return [load(wg_h.at[:, cols], wg.at[:, cols]), load(wu_h.at[:, cols], wu.at[:, cols])]

    first_loads = [load(tok_h, tok), load(g1_h, g1)]
    pair1 = [load_pair(wg1_h, wu1_h, wg1, wu1, c) for c in range(n_chunks)]
    down1_loads = load_rows(wd1_h, wd1, 4)
    mix_loads = [load(g2_h, g2), load(wf_h, wf)]
    q_loads = load_rows(wq_h, wq, 2)
    k_loads = load_rows(wk_h, wk, 2)
    v_loads = load_rows(wv_h, wv, 2)
    key_loads = [load(gc_h, gc), load(len_h, lens)] + load_rows(kc_h, kc, 1)
    val_loads = load_rows(vc_h, vc, 1)
    out_loads = load_rows(wo_h, wo, 2) + [load(g3_h, g3)]
    pair2 = [load_rows(wg2_h, wg2, 4) + load_rows(wu2_h, wu2, 4)] + [[]] * (n_chunks - 1)
    down2_loads = load_rows(wd2_h, wd2, 4)

    def wait_all(copies):
        for copy in copies:
            copy.wait()

    base_tp, base_kv = [0], [0]
    pending = []

    def tp_exchange(buffer):
        ex = Exchange("tp", n_tp, buffer, tp_send, tp_recv, base_tp[0])
        base_tp[0] += n_tp - 1
        return ex

    def kv_exchange(buffer):
        ex = Exchange("kv", n_kv, buffer, kv_send, kv_recv, base_kv[0])
        base_kv[0] += n_kv - 1
        return ex

    def begin(ex, window=None):
        ex.start(window)
        pending.append((ex, window))

    def total(buffer, count, rows=slice(None)):
        acc = buffer[0, rows].astype(F32)
        for j in range(1, count):
            acc = acc + buffer[j, rows].astype(F32)
        return acc

    lane = lax.broadcasted_iota(jnp.int32, (batch, LANES), 1)

    def kv_product(lhs, weight, xd):
        parts = KV_WINDOWS if model % (KV_WINDOWS * 256) == 0 else 1
        size = model // parts
        sent = []
        for i in range(parts):
            cols = slice(i * size, (i + 1) * size)
            xd[me_kv, :, cols] = dot(lhs, weight[:, cols]).astype(BF16)
            ex = kv_exchange(xd)
            window = None if parts == 1 else (i * size, size)
            begin(ex, window)
            sent.append((ex, window, cols))
        sums = []
        for ex, window, cols in sent:
            ex.wait_recv(window)
            sums.append(xd[0, :, cols].astype(F32))
            for j in range(1, n_kv):
                sums[-1] = sums[-1] + xd[j, :, cols].astype(F32)
        return jnp.concatenate(sums, axis=1)

    def half_step(rows, gain, pairs, wg, wu, down_loads, wd, x1, xs, xd, first):
        squares = jnp.sum(rows * rows, axis=1, keepdims=True)
        weighted = (rows * gain[...]).astype(BF16)
        xs[me_tp] = jnp.broadcast_to(squares, (batch, LANES))
        sq_ex = tp_exchange(xs)
        if first:
            pl.semaphore_wait(barrier, n_tp - 1 + n_kv - 1)
        begin(sq_ex)
        cuts = sorted({n_chunks * i // WINDOWS for i in range(WINDOWS + 1)})
        windows = []
        for lo, hi in zip(cuts[:-1], cuts[1:]):
            for c in range(lo, hi):
                wait_all(pairs[c])
                cols = pl.ds(c * cw, cw)
                both = jnp.concatenate([dot(weighted, wg[:, cols]), dot(weighted, wu[:, cols])], axis=0)
                x1[me_tp, :, cols] = both.astype(BF16)
            window = None if n_chunks == 1 else (lo * cw, (hi - lo) * cw)
            ex = tp_exchange(x1)
            begin(ex, window)
            windows.append((ex, window, slice(lo * cw, hi * cw)))
        sq_ex.wait_recv()
        scale = lax.rsqrt(total(xs, n_tp)[:, 0:1] / d_full + EPSILON)
        for ex, window, cols in windows:
            ex.wait_recv(window)
            acc = x1[0, :, cols].astype(F32)
            for j in range(1, n_tp):
                acc = acc + x1[j, :, cols].astype(F32)
            gate, up = scale * acc[:batch], scale * acc[batch:]
            hid[:, cols] = (gate / (1.0 + jnp.exp(-gate)) * up).astype(BF16)
        wait_all(down_loads)
        return (rows + 0.5 * kv_product(hid[...], wd, xd)).astype(BF16).astype(F32)

    wait_all(first_loads)
    after_first = half_step(
        tok[...].astype(F32), g1, pair1, wg1, wu1, down1_loads, wd1, x1a, xs1, xd1, True
    )

    squares = jnp.sum(after_first * after_first, axis=1, keepdims=True)
    wait_all(mix_loads)
    weighted = (after_first * g2[...]).astype(BF16)
    n_heads_all = wf.shape[0]
    forget = lax.dot_general(
        weighted, wf[...], (((1,), (1,)), ((), ())), preferred_element_type=F32
    )
    forget = jnp.concatenate([forget, jnp.zeros((batch, LANES - n_heads_all), F32)], axis=1)
    xs2[me_tp] = jnp.where(lane == LANES - 1, squares, forget)
    s_ex = tp_exchange(xs2)
    begin(s_ex)
    wait_all(q_loads)
    xq[me_tp] = dot(weighted, wq[...])
    q_ex = tp_exchange(xq)
    begin(q_ex)
    wait_all(k_loads)
    key_part = dot(weighted, wk[...])
    wait_all(v_loads)
    xkv[me_tp] = jnp.concatenate([key_part, dot(weighted, wv[...])], axis=0).astype(BF16)
    kv_ex = tp_exchange(xkv)
    begin(kv_ex)

    s_ex.wait_recv()
    small = total(xs2, n_tp)
    scale = lax.rsqrt(small[:, LANES - 1 :] / d_full + EPSILON)
    logits = scale * small
    log_all = jnp.minimum(logits, 0.0) - jnp.log(1.0 + jnp.exp(-jnp.abs(logits)))
    log_forget = log_all
    for k in range(1, n_kv):
        log_forget = jnp.where(
            me_kv == k, pltpu.roll(log_all, LANES - k * heads, 1), log_forget
        )
    q_ex.wait_recv()
    query = (scale * total(xq, n_tp)).astype(BF16).astype(F32)

    wait_all(key_loads)
    wait_all(val_loads)
    row_head = lax.broadcasted_iota(jnp.int32, (heads, width), 0)
    own_cols = row_head == lax.broadcasted_iota(jnp.int32, (heads, width), 1) // HEAD_DIM
    slots = me_tp * span + lax.broadcasted_iota(jnp.int32, (heads, span), 1)
    stat_row = lax.broadcasted_iota(jnp.int32, (heads, LANES), 0)
    stat_lane = lax.broadcasted_iota(jnp.int32, (heads, LANES), 1)
    half = LANES // 2
    all_scores = []
    for b in range(batch):
        spread = jnp.where(own_cols, query[b : b + 1, :], 0.0).astype(BF16)
        all_scores.append(
            lax.dot_general(spread, kc[b], (((1,), (1,)), ((), ())), preferred_element_type=F32)
        )
    all_probs = []
    for b in range(batch):
        scores = all_scores[b] * HEAD_DIM ** (-0.5) + gc[b]
        live = slots < lens[b]
        top = jnp.max(jnp.where(live, scores, MASKED), axis=1, keepdims=True)
        probs = jnp.where(live, jnp.exp(scores - top), 0.0)
        mass = jnp.sum(probs, axis=1, keepdims=True)
        all_probs.append(probs.astype(BF16))
        placed = jnp.where(
            stat_row == stat_lane, top, jnp.where(stat_row + half == stat_lane, mass, 0.0)
        )
        xs3[me_tp, b : b + 1, :] = jnp.sum(placed, axis=0, keepdims=True)
    st_ex = tp_exchange(xs3)
    begin(st_ex)
    for b in range(batch):
        mixed = dot(all_probs[b], vc[b])
        osum[b : b + 1, :] = jnp.sum(jnp.where(own_cols, mixed, 0.0), axis=0, keepdims=True)
    xo[me_tp] = osum[...].astype(BF16)
    o_ex = tp_exchange(xo)
    begin(o_ex)

    kv_ex.wait_recv()
    kv_sum = total(xkv, n_tp)
    key_new = (scale * kv_sum[:batch]).astype(BF16).astype(F32)
    value_new = (scale * kv_sum[batch:]).astype(BF16).astype(F32)
    own = jnp.zeros((batch, LANES), F32)
    for h in range(heads):
        cols = slice(h * HEAD_DIM, (h + 1) * HEAD_DIM)
        own = jnp.where(
            lane == h, jnp.sum(query[:, cols] * key_new[:, cols], axis=1, keepdims=True), own
        )
    own = own * HEAD_DIM ** (-0.5)

    st_ex.wait_recv()
    tops = [xs3[j] + log_forget for j in range(n_tp)]
    highest = own
    for t in tops:
        highest = jnp.maximum(highest, t)
    factors = [jnp.exp(t - highest) for t in tops]
    own_factor = jnp.exp(own - highest)
    denom = own_factor
    for j in range(n_tp):
        denom = denom + factors[j] * pltpu.roll(xs3[j], half, 1)
    own_factor = own_factor / denom
    factors = [f / denom for f in factors]
    o_ex.wait_recv()
    pieces = []
    for h in range(heads):
        cols = slice(h * HEAD_DIM, (h + 1) * HEAD_DIM)
        acc = own_factor[:, h : h + 1] * value_new[:, cols]
        for j in range(n_tp):
            acc = acc + factors[j][:, h : h + 1] * xo[j, :, cols].astype(F32)
        pieces.append(acc.astype(BF16))
    attended = jnp.concatenate(pieces, axis=1)
    wait_all(out_loads)
    residual_two = (after_first + kv_product(attended, wo, xd2)).astype(BF16).astype(F32)

    result = half_step(
        residual_two, g3, pair2, wg2, wu2, down2_loads, wd2, x1b, xs4, xd3, False
    )
    out_ref[...] = result.astype(out_ref.dtype)
    for ex, window in pending:
        ex.wait_send(window)


def on_device(n_tp, n_kv, *args):
    (tokens, pre_gain, gate_first, up_first, down_first, mix_gain, query_w, key_w, value_w,
     forget_w, key_cache, value_cache, gate_cache, lengths, out_w, post_gain, gate_second,
     up_second, down_second) = args
    batch, model = tokens.shape
    hidden = gate_first.shape[1]
    width = query_w.shape[1]
    span = key_cache.shape[1]
    heads = width // HEAD_DIM
    d_full = model * n_tp
    row = lambda v: v.reshape(1, v.shape[0])
    operands = [tokens, row(pre_gain), gate_first, up_first, down_first, row(mix_gain), query_w,
                key_w, value_w, forget_w.T, key_cache, value_cache, gate_cache, lengths, out_w,
                row(post_gain), gate_second, up_second, down_second]
    lengths_at = 13
    any_spec = pl.BlockSpec(memory_space=pl.ANY)
    in_specs = [any_spec] * len(operands)
    held = [pltpu.VMEM(a.shape, a.dtype) for i, a in enumerate(operands) if i != lengths_at]
    dims = (batch, model, width, hidden, span, heads, d_full)
    small = pltpu.VMEM((n_tp, batch, LANES), F32)
    cw = chunk_width(hidden)
    n_local = 2 * (hidden // cw) + 64
    tp_slots = (7 + 2 * WINDOWS) * (n_tp - 1)
    kv_slots = 3 * KV_WINDOWS * (n_kv - 1)
    scratch = held + [
        pltpu.VMEM((batch, hidden), BF16),
        pltpu.VMEM((batch, width), F32),
        pltpu.VMEM((n_tp, 2 * batch, hidden), BF16),
        pltpu.VMEM((n_tp, 2 * batch, hidden), BF16),
        small,
        small,
        small,
        pltpu.VMEM((n_tp, batch, width), F32),
        pltpu.VMEM((n_tp, 2 * batch, width), BF16),
        pltpu.VMEM((n_tp, batch, width), BF16),
        pltpu.VMEM((n_kv, batch, model), BF16),
        pltpu.VMEM((n_kv, batch, model), BF16),
        pltpu.VMEM((n_kv, batch, model), BF16),
        small,
        pltpu.SMEM((lengths.shape[0],), lengths.dtype),
        pltpu.SemaphoreType.DMA((n_local,)),
        pltpu.SemaphoreType.DMA((tp_slots,)),
        pltpu.SemaphoreType.DMA((tp_slots,)),
        pltpu.SemaphoreType.DMA((kv_slots,)),
        pltpu.SemaphoreType.DMA((kv_slots,)),
    ]
    return pl.pallas_call(
        functools.partial(body, n_tp, n_kv, dims),
        out_shape=jax.ShapeDtypeStruct(tokens.shape, tokens.dtype),
        in_specs=in_specs,
        out_specs=pl.BlockSpec(memory_space=pltpu.VMEM),
        scratch_shapes=scratch,
        compiler_params=pltpu.CompilerParams(
            collective_id=0, has_side_effects=True, vmem_limit_bytes=62 * 1024 * 1024
        ),
    )(*operands)


def solution(mesh):
    placed = (
        P("grp", "tp"),
        P("tp"),
        P("tp", "kv"),
        P("tp", "kv"),
        P("kv", "tp"),
        P("tp"),
        P("tp", "kv"),
        P("tp", "kv"),
        P("tp", "kv"),
        P("tp", None),
        P("grp", "tp", "kv"),
        P("grp", "tp", "kv"),
        P("grp", "kv", "tp"),
        P("grp"),
        P("kv", "tp"),
        P("tp"),
        P("tp", "kv"),
        P("tp", "kv"),
        P("kv", "tp"),
    )
    return jax.shard_map(
        functools.partial(on_device, mesh.shape["tp"], mesh.shape["kv"]),
        mesh=mesh,
        in_specs=placed,
        out_specs=P("grp", "tp"),
        check_vma=False,
    )
```
